32 devices in a mesh: sp: 8 (over z, x), tp: 4 (over y, core).
Axes of the slice: x: 2, y: 2, z: 4, core: 2. Of those that a mesh axis runs over, the one named last changes fastest.
Arguments:
- tokens: bfloat16 [4096, 2048], P(('sp', 'tp')), may hold values from -8 to 8
- in_gain: float32 [2048], replicated, may hold values from 0.1 to 1.9
- w_conv_val: bfloat16 [2048, 1024], P('sp', 'tp'), may hold values from -0.125 to 0.125
- w_conv_gate: bfloat16 [2048, 1024], P('sp', 'tp'), may hold values from -0.125 to 0.125
- w_query: bfloat16 [2048, 1024], P('sp', 'tp'), may hold values from -1 to 1
- w_key: bfloat16 [2048, 256], P('sp', 'tp'), may hold values from -1 to 1
- value_weight: bfloat16 [2048, 256], P('sp', 'tp'), may hold values from -0.125 to 0.125
- conv_taps: float32 [31, 1024], P(None, 'tp'), may hold values from -1 to 1
- conv_bias: float32 [1024], P('tp'), may hold values from -3 to 3
- norm_gain: float32 [1024], P('tp'), may hold values from 0.1 to 1.9
- norm_bias: float32 [1024], P('tp'), may hold values from -3 to 3
- head_sink_logit: float32 [16], P('tp'), may hold values from 4 to 7
- w_out_conv: bfloat16 [1024, 2048], P('tp', 'sp'), may hold values from -0.125 to 0.125
- w_out_attn: bfloat16 [1024, 2048], P('tp', 'sp'), may hold values from -0.125 to 0.125
Outputs:
- mixed: bfloat16 [4096, 2048], P(('sp', 'tp'))
- log_total: float32 [4096, 16], P('sp', 'tp')
The draws below stay inside these ranges and needn't reach their ends.
All inputs are finite; a program needn't handle non-finite values.
Results may differ from the reference program's by a relative error of at most 0.012.
Values may be sent and summed in bfloat16 or wider, within the bound.
A program may use at most 64 MiB of HBM per device.

```python
import math
import jax
import jax.numpy as jnp
from jax import lax

MODEL_WIDTH = 2048
CONV = 1024
QUERY_HEADS = 16
KEY_VALUE_HEADS = 4
HEAD_WIDTH = 64
CONV_TAPS = 31
WINDOW_REACH = 128
TOK_DEV = 512
TOKENS = 4096


def planted_parts(key):
    random_seed_key = jax.random.fold_in(key, 101)
    direction = jnp.where(jax.random.bernoulli(jax.random.fold_in(random_seed_key, 1), 0.5, (MODEL_WIDTH,)), 1.0, -1.0).astype(jnp.float32)
    mask_pattern = jnp.where(jax.random.bernoulli(jax.random.fold_in(random_seed_key, 2), 0.5, (KEY_VALUE_HEADS, HEAD_WIDTH)), 1.0, -1.0).astype(jnp.float32)
    strength = math.sqrt(288.0) / HEAD_WIDTH ** 0.25
    return (direction, mask_pattern, strength)


def draw_tokens(key, part):
    direction, mask_pattern, strength = planted_parts(key)
    jitter = jnp.clip(jax.random.normal(jax.random.fold_in(key, 201), (TOKENS, MODEL_WIDTH), jnp.float32), -4.0, 4.0)
    levels = jnp.exp(jax.random.uniform(jax.random.fold_in(key, 202), (TOKENS, 1), jnp.float32, math.log(0.7), math.log(4.0)))
    chosen = jax.random.bernoulli(jax.random.fold_in(key, 203), 0.125, (TOKENS, 1))
    result = jnp.where(chosen, levels * direction[None, :] + jitter, jitter)
    return result.astype(jnp.bfloat16)


def draw_w_query(key, part):
    direction, mask_pattern, strength = planted_parts(key)
    random_draws = jnp.clip(jax.random.normal(jax.random.fold_in(key, 301), (MODEL_WIDTH, QUERY_HEADS * HEAD_WIDTH), jnp.float32), -4.0, 4.0) * MODEL_WIDTH ** (-0.5)
    column_list = jnp.repeat(mask_pattern, QUERY_HEADS // KEY_VALUE_HEADS, axis=0).reshape(QUERY_HEADS * HEAD_WIDTH)
    result = random_draws + strength / MODEL_WIDTH * direction[:, None] * column_list[None, :]
    return result.astype(jnp.bfloat16)


def draw_w_key(key, part):
    direction, mask_pattern, strength = planted_parts(key)
    random_draws = jnp.clip(jax.random.normal(jax.random.fold_in(key, 401), (MODEL_WIDTH, KEY_VALUE_HEADS * HEAD_WIDTH), jnp.float32), -4.0, 4.0) * MODEL_WIDTH ** (-0.5)
    column_list = mask_pattern.reshape(KEY_VALUE_HEADS * HEAD_WIDTH)
    result = random_draws + strength / MODEL_WIDTH * direction[:, None] * column_list[None, :]
    return result.astype(jnp.bfloat16)


def shard_levels(own_key, dims, split, smallest, high):
    def one(dim, parts):
        steps = jax.random.uniform(jax.random.fold_in(jax.random.fold_in(own_key, 6), dim), (parts,), jnp.float32, smallest / len(split), high / len(split))
        return jnp.repeat(jnp.exp(steps), dims[dim] // parts).reshape((-1,) + (1,) * (len(dims) - dim - 1))

    factor_of = one(*split[0])
    for cut in split[1:]:
        factor_of = factor_of * one(*cut)
    return factor_of


def centred(key, extent, scale, most, shards=(), held_as=jnp.bfloat16):
    entries = scale * jax.random.normal(key, extent, jnp.float32)
    if shards:
        entries = entries * shard_levels(key, extent, shards, -0.22, 0.18)
    return jnp.clip(entries, -most, most).astype(held_as)


def setup_inputs(seed: int = 0) -> dict:
    splits = jax.random.split(jax.random.key(seed), 15)
    return {
        "tokens": draw_tokens(jax.random.fold_in(splits[14], 71), 0),
        "in_gain": jnp.clip(1.0 + 0.18 * jax.random.normal(splits[1], (MODEL_WIDTH,), jnp.float32), 0.1, 1.9),
        "w_conv_val": centred(splits[2], (MODEL_WIDTH, CONV), MODEL_WIDTH ** -0.5, 0.125, ((0, 8), (1, 4))),
        "w_conv_gate": centred(splits[3], (MODEL_WIDTH, CONV), MODEL_WIDTH ** -0.5, 0.125, ((0, 8), (1, 4))),
        "w_query": draw_w_query(jax.random.fold_in(splits[14], 71), 0),
        "w_key": draw_w_key(jax.random.fold_in(splits[14], 71), 0),
        "value_weight": centred(splits[6], (MODEL_WIDTH, KEY_VALUE_HEADS * HEAD_WIDTH), MODEL_WIDTH ** -0.5, 0.125, ((0, 8), (1, 4))),
        "conv_taps": centred(splits[7], (CONV_TAPS, CONV), CONV_TAPS ** -0.5, 1.0, ((1, 4),), jnp.float32),
        "conv_bias": centred(splits[8], (CONV,), 0.5, 3.0, ((0, 4),), jnp.float32),
        "norm_gain": jnp.clip(1.0 + 0.18 * jax.random.normal(splits[9], (CONV,), jnp.float32), 0.1, 1.9),
        "norm_bias": centred(splits[10], (CONV,), 0.5, 3.0, ((0, 4),), jnp.float32),
        "head_sink_logit": jnp.clip(4.0 + 3.0 * jax.random.uniform(splits[11], (QUERY_HEADS,), jnp.float32) ** shard_levels(splits[11], (QUERY_HEADS,), ((0, 4),), -0.2, 0.2), 4.0, 7.0),
        "w_out_conv": centred(splits[12], (CONV, MODEL_WIDTH), (CONV + QUERY_HEADS * HEAD_WIDTH) ** -0.5, 0.125, ((0, 4), (1, 8))),
        "w_out_attn": centred(splits[13], (QUERY_HEADS * HEAD_WIDTH, MODEL_WIDTH), (CONV + QUERY_HEADS * HEAD_WIDTH) ** -0.5, 0.125, ((0, 4), (1, 8))),
    }


def reference(tokens, in_gain, w_conv_val, w_conv_gate, w_query, w_key, value_weight, conv_taps, conv_bias, norm_gain, norm_bias, head_sink_logit, w_out_conv, w_out_attn):
    every_row = tokens.shape[0]
    flt = tokens.astype(jnp.float32)
    normed = (flt * lax.rsqrt(lax.optimization_barrier(jnp.mean(flt * flt, axis=-1, keepdims=True)) + 1e-06) * in_gain).astype(jnp.bfloat16)
    val_part = jnp.dot(normed, w_conv_val, preferred_element_type=jnp.float32)
    gate_part = jnp.dot(normed, w_conv_gate, preferred_element_type=jnp.float32)
    glu = (val_part * jax.nn.sigmoid(gate_part)).astype(jnp.bfloat16)
    half = CONV_TAPS // 2
    padded = jnp.pad(glu, ((half, half), (0, 0)))
    filtered = jnp.zeros(glu.shape, jnp.float32) + conv_bias
    for offset in range(CONV_TAPS):
        filtered = filtered + padded[offset:offset + every_row].astype(jnp.float32) * conv_taps[offset]
    center = lax.optimization_barrier(jnp.mean(filtered, axis=-1, keepdims=True))
    spread = lax.optimization_barrier(jnp.mean((filtered - center) ** 2, axis=-1, keepdims=True))
    conv_out = jax.nn.silu((filtered - center) * lax.rsqrt(spread + 1e-05) * norm_gain + norm_bias).astype(jnp.bfloat16)
    query_matrix = jnp.dot(normed, w_query, preferred_element_type=jnp.float32).astype(jnp.bfloat16)
    key = jnp.dot(normed, w_key, preferred_element_type=jnp.float32).astype(jnp.bfloat16)
    value_matrix = jnp.dot(normed, value_weight, preferred_element_type=jnp.float32).astype(jnp.bfloat16)
    query_groups = QUERY_HEADS // KEY_VALUE_HEADS
    query4_grouped = query_matrix.reshape(every_row, KEY_VALUE_HEADS, query_groups, HEAD_WIDTH)
    padded_keys = jnp.pad(key.reshape(every_row, KEY_VALUE_HEADS, HEAD_WIDTH), ((WINDOW_REACH, WINDOW_REACH), (0, 0), (0, 0)))
    padded_values = jnp.pad(value_matrix.reshape(every_row, KEY_VALUE_HEADS, HEAD_WIDTH), ((WINDOW_REACH, WINDOW_REACH), (0, 0), (0, 0)))
    block = TOK_DEV
    sink_column = head_sink_logit.reshape(KEY_VALUE_HEADS, query_groups, 1)

    def attend(index):
        first = (index * block).astype(jnp.int32)
        qblock = lax.dynamic_slice_in_dim(query4_grouped, first, block, 0).astype(jnp.float32)
        kblock = lax.dynamic_slice_in_dim(padded_keys, first, block + 2 * WINDOW_REACH, 0).astype(jnp.float32)
        vblock = lax.dynamic_slice_in_dim(padded_values, first, block + 2 * WINDOW_REACH, 0).astype(jnp.float32)
        scores = jnp.einsum('qkgd,jkd->kgqj', qblock, kblock) * HEAD_WIDTH ** (-0.5)
        qpos = first + jnp.arange(block, dtype=jnp.int32)
        kpos = first - WINDOW_REACH + jnp.arange(block + 2 * WINDOW_REACH, dtype=jnp.int32)
        valid = (jnp.abs(qpos[:, None] - kpos[None, :]) <= WINDOW_REACH) & (kpos[None, :] >= 0) & (kpos[None, :] < every_row)
        masked = jnp.where(valid, scores, -1e+30)
        top = jnp.maximum(lax.optimization_barrier(jnp.max(masked, axis=-1)), sink_column)
        expd = jnp.where(valid, jnp.exp(masked - top[..., None]), 0.0)
        total = lax.optimization_barrier(jnp.sum(expd, axis=-1)) + jnp.exp(sink_column - top)
        probs = (expd / total[..., None]).astype(jnp.bfloat16)
        attended = jnp.einsum('kgqj,jkd->qkgd', probs.astype(jnp.float32), vblock).astype(jnp.bfloat16)
        log_block = (top + jnp.log(total)).reshape(QUERY_HEADS, block).T
        return (attended.reshape(block, QUERY_HEADS * HEAD_WIDTH), log_block)
    attended, log_total = lax.map(attend, jnp.arange(every_row // block, dtype=jnp.int32))
    attended = attended.reshape(every_row, QUERY_HEADS * HEAD_WIDTH)
    log_total = log_total.reshape(every_row, QUERY_HEADS)
    features = jnp.concatenate([conv_out, attended], axis=1)
    weights_all = jnp.concatenate([w_out_conv, w_out_attn], axis=0)
    mixed = jnp.dot(features, weights_all, preferred_element_type=jnp.float32).astype(jnp.bfloat16)
    return (mixed, log_total)
```

```python
import functools

import jax
import jax.numpy as jnp
from jax import lax
from jax.experimental import pallas as pl
from jax.experimental.pallas import tpu as pltpu
from jax.sharding import PartitionSpec as P

WINDOW_REACH = 128


def with_halo(cells, sides, width):
    for axis, dim in sides:
        count = lax.axis_size(axis)
        ends = count - 1
        head = lax.slice_in_dim(cells, 0, width, axis=dim)
        tail = lax.slice_in_dim(cells, cells.shape[dim] - width, cells.shape[dim], axis=dim)
        cells = jnp.concatenate(
            [
                lax.ppermute(tail, axis, [(i, (i + 1) % count) for i in range(ends)]),
                cells,
                lax.ppermute(head, axis, [((i + 1) % count, i) for i in range(ends)]),
            ],
            axis=dim,
        )
    return cells


def on_device(
    tokens,
    in_gain,
    w_conv_val,
    w_conv_gate,
    w_query,
    w_key,
    value_weight,
    conv_taps,
    conv_bias,
    norm_gain,
    norm_bias,
    head_sink_logit,
    w_out_conv,
    w_out_attn,
):
    flt = tokens.astype(jnp.float32)
    normed = (
        flt * lax.rsqrt(jnp.mean(flt * flt, axis=-1, keepdims=True) + 1e-06) * in_gain
    ).astype(jnp.bfloat16)
    val_full, gate_full, query_full, key_full, value_full = (
        lax.all_gather(w_conv_val, "sp", axis=0, tiled=True),
        lax.all_gather(w_conv_gate, "sp", axis=0, tiled=True),
        lax.all_gather(w_query, "sp", axis=0, tiled=True),
        lax.all_gather(w_key, "sp", axis=0, tiled=True),
        lax.all_gather(value_weight, "sp", axis=0, tiled=True),
    )
    joined = jnp.concatenate([val_full, gate_full, query_full, key_full, value_full], axis=1)
    projected = jnp.dot(
        lax.all_gather(normed, "tp", axis=0, tiled=True), joined, preferred_element_type=jnp.float32
    )
    chans = val_full.shape[1]
    qwidth = query_full.shape[1]
    kwidth = key_full.shape[1]
    length = projected.shape[0]
    glu = (projected[:, :chans] * jax.nn.sigmoid(projected[:, chans : 2 * chans])).astype(
        jnp.bfloat16
    )
    base = 2 * chans
    query_matrix = projected[:, base : base + qwidth].astype(jnp.bfloat16)
    key = projected[:, base + qwidth : base + qwidth + kwidth].astype(jnp.bfloat16)
    value_matrix = projected[:, base + qwidth + kwidth :].astype(jnp.bfloat16)
    taps = conv_taps.shape[0]
    half = taps // 2
    padded = with_halo(glu, (("sp", 0),), half)
    filtered = jnp.zeros(glu.shape, jnp.float32) + conv_bias
    for offset in range(taps):
        filtered = (
            filtered + padded[offset : offset + length].astype(jnp.float32) * conv_taps[offset]
        )
    sums, squares = lax.psum(
        (jnp.sum(filtered, axis=-1), jnp.sum(filtered * filtered, axis=-1)), "tp"
    )
    count = chans * lax.axis_size("tp")
    center = (sums / count)[:, None]
    spread = (squares / count)[:, None] - center * center
    conv_out = jax.nn.silu(
        (filtered - center) * lax.rsqrt(spread + 1e-05) * norm_gain + norm_bias
    ).astype(jnp.bfloat16)
    heads_here = head_sink_logit.shape[0]
    head_size = qwidth // heads_here
    kv_here = kwidth // head_size
    query_groups = heads_here // kv_here
    stacked = jnp.stack([key, value_matrix], axis=0)
    banded = with_halo(stacked, (("sp", 1),), WINDOW_REACH)
    span = length + 2 * WINDOW_REACH
    key_band = banded[0].reshape(span, kv_here, head_size)
    value_band = banded[1].reshape(span, kv_here, head_size)
    query4_grouped = query_matrix.reshape(length, kv_here, query_groups, head_size)
    scores = jnp.einsum(
        "qkgd,jkd->kgqj", query4_grouped, key_band, preferred_element_type=jnp.float32
    ) * head_size ** (-0.5)
    offset_pos = lax.axis_index("sp") * length
    seq_len = length * lax.axis_size("sp")
    qpos = offset_pos + jnp.arange(length, dtype=jnp.int32)
    kpos = offset_pos - WINDOW_REACH + jnp.arange(span, dtype=jnp.int32)
    valid = (
        (jnp.abs(qpos[:, None] - kpos[None, :]) <= WINDOW_REACH)
        & (kpos[None, :] >= 0)
        & (kpos[None, :] < seq_len)
    )
    sink_column = head_sink_logit.reshape(kv_here, query_groups, 1)
    masked = jnp.where(valid, scores, -1e30)
    top = jnp.maximum(jnp.max(masked, axis=-1), sink_column)
    expd = jnp.where(valid, jnp.exp(masked - top[..., None]), 0.0)
    total = jnp.sum(expd, axis=-1) + jnp.exp(sink_column - top)
    probs = (expd / total[..., None]).astype(jnp.bfloat16)
    attended = jnp.einsum(
        "kgqj,jkd->qkgd", probs, value_band, preferred_element_type=jnp.float32
    ).astype(jnp.bfloat16)
    attended = attended.reshape(length, qwidth)
    log_total = (top + jnp.log(total)).reshape(heads_here, length).T
    out_conv_cols, out_attn_cols = (
        lax.all_gather(w_out_conv, "sp", axis=1, tiled=True),
        lax.all_gather(w_out_attn, "sp", axis=1, tiled=True),
    )
    out_rows = jnp.concatenate([out_conv_cols, out_attn_cols], axis=0)
    features = jnp.concatenate([conv_out, attended], axis=1)
    mixed = lax.psum_scatter(
        jnp.dot(features, out_rows, preferred_element_type=jnp.float32).astype(jnp.bfloat16),
        "tp",
        scatter_dimension=0,
        tiled=True,
    )
    return (mixed, log_total)


BF = jnp.bfloat16
F32 = jnp.float32


def fused_kernel(
    n, x_hbm, gain, wval, wgate, wquery, wkv, taps, cbias, ngain, nbias, sink, woc, woa,
    mixed, logt,
    tok, nrm, wq, wc, wo, accq, accc, qb, band, glu, filt, stat, feat, part,
    p1s, p1r, p2s, p2r, own,
    lsem, tsem, trec, rsem, rrec, hsem, hrec, ssem, srec, asem, arec, bsem, brec,
):
    sp = lax.axis_index("sp")
    t = lax.axis_index("tp")
    half = n // 2
    tl, width = x_hbm.shape
    length = 4 * tl
    kb = wval.shape[0]
    chans = wval.shape[1]
    qwidth = wquery.shape[1]
    kvw = wkv.shape[1]
    hd = kvw // 2
    heads = sink.shape[1]
    ob = woc.shape[1]
    reach = WINDOW_REACH
    y, c = t // 2, t % 2
    core_peer = y * 2 + 1 - c
    y_peer = (1 - y) * 2 + c
    far_peer = (1 - y) * 2 + 1 - c
    xbit, zpos = sp % 2, sp // 2
    pos = (1 - xbit) * zpos + xbit * (n - 1 - zpos)

    def at_pos(q):
        q = (q + 2 * n) % n
        hi = q // half
        return (1 - hi) * (2 * q) + hi * (2 * (n - 1 - q) + 1)

    right, left = at_pos(pos + 1), at_pos(pos - 1)
    nxt, prv = (sp + 1) % n, (sp + n - 1) % n

    def rows(o, size):
        return pl.ds(pl.multiple_of(o * size, size), size)

    local = [
        pltpu.make_async_copy(x_hbm, tok.at[rows(t, tl)], lsem.at[0]),
        pltpu.make_async_copy(wquery, wq.at[rows(sp, kb), pl.ds(0, qwidth)], lsem.at[1]),
        pltpu.make_async_copy(wkv, wq.at[rows(sp, kb), pl.ds(qwidth, kvw)], lsem.at[2]),
        pltpu.make_async_copy(wval, wc.at[rows(sp, kb), pl.ds(0, chans)], lsem.at[3]),
        pltpu.make_async_copy(wgate, wc.at[rows(sp, kb), pl.ds(chans, chans)], lsem.at[4]),
        pltpu.make_async_copy(woc, wo.at[sp, pl.ds(0, chans)], lsem.at[5]),
        pltpu.make_async_copy(woa, wo.at[sp, pl.ds(chans, qwidth)], lsem.at[6]),
    ]
    for cp in local:
        cp.start()
    barrier = pltpu.get_barrier_semaphore()
    for dev in (right, left, nxt, prv):
        pl.semaphore_signal(
            barrier, inc=1, device_id={"sp": dev}, device_id_type=pl.DeviceIdType.MESH
        )
    for dev in (core_peer, y_peer, far_peer):
        pl.semaphore_signal(
            barrier, inc=1, device_id={"tp": dev}, device_id_type=pl.DeviceIdType.MESH
        )
    pl.semaphore_wait(barrier, 7)

    sent = []

    def remote(src, dst, ss, rs, dev):
        cp = pltpu.make_async_remote_copy(
            src_ref=src, dst_ref=dst, send_sem=ss, recv_sem=rs, device_id=dev,
            device_id_type=pl.DeviceIdType.MESH,
        )
        cp.start()
        sent.append(cp)
        return cp

    ring = {}

    def block_ref(k, o, h):
        if k == 0:
            return wq.at[pl.ds(pl.multiple_of(o * kb + h * (kb // 2), kb // 2), kb // 2)]
        if k == 1:
            return wc.at[pl.ds(pl.multiple_of(o * kb + h * (kb // 2), kb // 2), kb // 2)]
        depth = wo.shape[1] // 2
        return wo.at[o, pl.ds(h * depth, depth)]

    def ring_event(k, s):
        for h in (0, 1):
            for d in (0, 1):
                if s > 1:
                    ring[k, d, s - 1, h].wait_recv()
                if s < half or h == d:
                    o = at_pos(pos - (s - 1) if d == 0 else pos + (s - 1))
                    ref = block_ref(k, o, h)
                    ring[k, d, s, h] = remote(
                        ref, ref, rsem.at[k, d, s - 1, h], rrec.at[k, d, s - 1, h],
                        {"sp": right if d == 0 else left},
                    )

    def ring_last(k):
        for d in (0, 1):
            ring[k, d, half, d].wait_recv()

    def owners(s):
        if s == 0:
            return [sp]
        if s == half:
            return [at_pos(pos + half)]
        return [at_pos(pos - s), at_pos(pos + s)]

    local[1].wait()
    local[2].wait()
    ring_event(0, 1)
    local[0].wait()
    hl = tl // 2
    tokcp = {}

    def tok_send(slot, h, e, dev):
        ref = tok.at[pl.ds(pl.multiple_of(slot * tl + h * hl, hl), hl)]
        tokcp[e, h] = remote(ref, ref, tsem.at[e, h], trec.at[e, h], {"tp": dev})

    for h in (0, 1):
        tok_send(t, h, 0, y_peer)
    for h in (0, 1):
        tok_send(t, h, 1, core_peer)
    for cp in local[3:]:
        cp.wait()

    def norm_rows(slot):
        step = 32

        def body(i, carry):
            r = pl.ds(pl.multiple_of(slot * tl + i * step, step), step)
            flt = tok[r, :].astype(F32)
            scale = lax.rsqrt(jnp.mean(flt * flt, axis=-1, keepdims=True) + 1e-06)
            nrm[r, :] = (flt * scale * gain[...]).astype(BF)
            return carry

        lax.fori_loop(0, tl // step, body, 0)

    norm_rows(t)
    for h in (0, 1):
        tokcp[1, h].wait_recv()
    norm_rows(core_peer)
    ring_event(0, 2)
    for h in (0, 1):
        tokcp[0, h].wait_recv()
        tok_send(y_peer, h, 2, core_peer)
        if h == 0:
            ring_event(0, 3)
    norm_rows(y_peer)
    ring_event(0, 4) if half >= 4 else None
    ring_event(1, 1)
    for h in (0, 1):
        tokcp[2, h].wait_recv()
    norm_rows(far_peer)

    def project(acc, w, o, first):
        res = jnp.dot(
            nrm[:, pl.ds(pl.multiple_of(o * kb, kb), kb)], w[rows(o, kb), :],
            preferred_element_type=F32,
        )
        acc[...] = res if first else acc[...] + res

    def project_all(acc, w):
        project(acc, w, 0, True)

        def body(o, carry):
            project(acc, w, o, False)
            return carry

        lax.fori_loop(1, n, body, 0)

    ring_last(0)
    project_all(accq, wq)
    qb[...] = accq[:, 0:qwidth].astype(BF)
    band[pl.ds(reach, length), :] = accq[:, qwidth : qwidth + kvw].astype(BF)
    kv_up = remote(
        band.at[pl.ds(length, reach)], band.at[pl.ds(0, reach)], hsem.at[0], hrec.at[0],
        {"sp": nxt},
    )
    kv_down = remote(
        band.at[pl.ds(reach, reach)], band.at[pl.ds(length + reach, reach)], hsem.at[1],
        hrec.at[1], {"sp": prv},
    )
    seq_len = length * n

    def attend(b):
        blk = reach
        span = blk + 2 * reach
        kk = band[pl.ds(b * blk, span), 0:hd]
        vv = band[pl.ds(b * blk, span), hd:kvw]
        ri = lax.broadcasted_iota(jnp.int32, (blk, span), 0)
        ci = lax.broadcasted_iota(jnp.int32, (blk, span), 1)
        kp = sp * length + b * blk - reach + ci
        valid = (ci >= ri) & (ci <= ri + 2 * reach) & (kp >= 0) & (kp < seq_len)
        for h in range(heads):
            q = qb[pl.ds(b * blk, blk), h * hd : (h + 1) * hd]
            s = lax.dot_general(
                q, kk, (((1,), (1,)), ((), ())), preferred_element_type=F32
            ) * hd ** (-0.5)
            s = jnp.where(valid, s, -1e30)
            sk = sink[0:1, h : h + 1]
            top = jnp.maximum(jnp.max(s, axis=-1, keepdims=True), sk)
            e = jnp.where(valid, jnp.exp(s - top), 0.0)
            total = jnp.sum(e, axis=-1, keepdims=True) + jnp.exp(sk - top)
            p = (e * (1.0 / total)).astype(BF)
            a = jnp.dot(p, vv, preferred_element_type=F32).astype(BF)
            feat[pl.ds(b * blk, blk), chans + h * hd : chans + (h + 1) * hd] = a
            logt[pl.ds(b * blk, blk), h : h + 1] = top + jnp.log(total)

    nblk = length // reach
    ring_event(1, 2)
    for b in range(1, nblk - 1):
        attend(b)
    ring_event(1, 3)
    kv_up.wait_recv()
    kv_down.wait_recv()
    attend(0)
    attend(nblk - 1)
    ring_event(1, 4)
    ring_event(2, 1)
    ring_last(1)
    project_all(accc, wc)
    pad = 16
    glu[pl.ds(pad, length), :] = (
        (accc[:, 0:chans] * jax.nn.sigmoid(accc[:, chans : 2 * chans])).astype(BF).astype(F32)
    )
    g_up = remote(
        glu.at[pl.ds(length, pad)], glu.at[pl.ds(0, pad)], hsem.at[2], hrec.at[2], {"sp": nxt}
    )
    g_down = remote(
        glu.at[pl.ds(pad, pad)], glu.at[pl.ds(length + pad, pad)], hsem.at[3], hrec.at[3],
        {"sp": prv},
    )
    ring_event(2, 2)
    g_up.wait_recv()
    g_down.wait_recv()

    @pl.when(sp == 0)
    def _():
        glu[pl.ds(0, pad), :] = jnp.zeros((pad, chans), F32)

    @pl.when(sp == n - 1)
    def _():
        glu[pl.ds(length + pad, pad), :] = jnp.zeros((pad, chans), F32)

    ntaps = taps.shape[0]
    off = pad - ntaps // 2
    cstep = 64

    def conv_rows(r0):
        acc = jnp.zeros((cstep, chans), F32) + cbias[...]
        for j in range(ntaps):
            acc = acc + glu[pl.ds(r0 + off + j, cstep), :] * taps[pl.ds(j, 1), :]
        filt[pl.ds(r0, cstep), :] = acc

    for i in range(length // cstep):
        conv_rows(i * cstep)
    lane = lax.broadcasted_iota(jnp.int32, (128, 128), 1)
    for b in range(length // 128):
        f = filt[pl.ds(b * 128, 128), :]
        s1 = jnp.sum(f, axis=-1, keepdims=True)
        s2 = jnp.sum(f * f, axis=-1, keepdims=True)
        tile = jnp.where(lane == 0, s1, jnp.where(lane == 1, s2, 0.0))
        stat[pl.ds(t, 1), :, pl.ds(b * 128, 128)] = jnp.transpose(tile)[None, 0:8, :]
    scp = []
    for e, dev in enumerate((y_peer, far_peer, core_peer)):
        scp.append(remote(stat.at[t], stat.at[t], ssem.at[e], srec.at[e], {"tp": dev}))
    ring_event(2, 3)
    for cp in scp:
        cp.wait_recv()
    count = chans * 4
    for b in range(length // 128):
        cols = pl.ds(b * 128, 128)
        tot = (stat[0, :, cols] + stat[1, :, cols] + stat[2, :, cols] + stat[3, :, cols]) / count
        tt = jnp.transpose(jnp.concatenate([tot] * 16, axis=0))
        center = tt[:, 0:1]
        spread = tt[:, 1:2] - center * center
        u = (filt[pl.ds(b * 128, 128), :] - center) * lax.rsqrt(spread + 1e-05)
        u = u * ngain[...] + nbias[...]
        feat[pl.ds(b * 128, 128), 0:chans] = (u * jax.nn.sigmoid(u)).astype(BF)

    acp, bcp = {}, {}
    order = []

    def emit(o):
        i = len(order)
        order.append(o)
        part[...] = jnp.dot(feat[...], wo[o], preferred_element_type=F32)
        p1s[i, pl.ds(0, tl), :] = part[rows(core_peer, tl), :].astype(BF)
        p1s[i, pl.ds(tl, tl), :] = part[rows(far_peer, tl), :].astype(BF)
        acp[i] = remote(p1s.at[i], p1r.at[i], asem.at[i], arec.at[i], {"tp": core_peer})
        own[i, pl.ds(0, tl), :] = part[rows(t, tl), :]
        own[i, pl.ds(tl, tl), :] = part[rows(y_peer, tl), :]

    def cross(i):
        acp[i].wait_recv()
        p2s[i] = (own[i, pl.ds(tl, tl), :] + p1r[i, pl.ds(tl, tl), :].astype(F32)).astype(BF)
        bcp[i] = remote(p2s.at[i], p2r.at[i], bsem.at[i], brec.at[i], {"tp": y_peer})

    def finish(i):
        bcp[i].wait_recv()
        mixed[:, rows(order[i], ob)] = (
            own[i, pl.ds(0, tl), :] + p1r[i, pl.ds(0, tl), :].astype(F32)
            + p2r[i].astype(F32)
        ).astype(BF)

    def out_step(s):
        for o in owners(s):
            emit(o)
            if len(order) >= 2:
                cross(len(order) - 2)

    for s in range(half - 1):
        out_step(s)
    ring_event(2, 4)
    out_step(half - 1)
    ring_last(2)
    out_step(half)
    cross(n - 1)
    for i in range(n):
        finish(i)
    for cp in sent:
        cp.wait_send()


def layer(
    n, parts, tokens, in_gain, w_conv_val, w_conv_gate, w_query, w_key, value_weight, conv_taps,
    conv_bias, norm_gain, norm_bias, head_sink_logit, w_out_conv, w_out_attn,
):
    tl, width = tokens.shape
    kb, chans = w_conv_val.shape
    qwidth = w_query.shape[1]
    kvw = 2 * w_key.shape[1]
    heads = head_sink_logit.shape[0]
    ob = w_out_conv.shape[1]
    fits = (
        parts == 4 and n == 8 and tl % 128 == 0 and kb % 128 == 0 and ob % 128 == 0
        and chans % 128 == 0 and kvw == 128 and qwidth == heads * kvw // 2
        and conv_taps.shape[0] <= 33
    )
    if not fits:
        return on_device(
            tokens, in_gain, w_conv_val, w_conv_gate, w_query, w_key, value_weight, conv_taps,
            conv_bias, norm_gain, norm_bias, head_sink_logit, w_out_conv, w_out_attn,
        )
    length = 4 * tl
    half = n // 2
    wkv = jnp.concatenate([w_key, value_weight], axis=1)
    vm = pl.BlockSpec(memory_space=pltpu.VMEM)
    hb = pl.BlockSpec(memory_space=pl.ANY)
    dma = pltpu.SemaphoreType.DMA
    return pl.pallas_call(
        functools.partial(fused_kernel, n),
        out_shape=(
            jax.ShapeDtypeStruct((tl, width), BF),
            jax.ShapeDtypeStruct((length, heads), F32),
        ),
        in_specs=[hb, vm, hb, hb, hb, hb, vm, vm, vm, vm, vm, hb, hb],
        out_specs=(vm, vm),
        scratch_shapes=[
            pltpu.VMEM((length, width), BF),
            pltpu.VMEM((length, width), BF),
            pltpu.VMEM((n * kb, qwidth + kvw), BF),
            pltpu.VMEM((n * kb, 2 * chans), BF),
            pltpu.VMEM((n, chans + qwidth, ob), BF),
            pltpu.VMEM((length, qwidth + kvw), F32),
            pltpu.VMEM((length, 2 * chans), F32),
            pltpu.VMEM((length, qwidth), BF),
            pltpu.VMEM((length + 2 * WINDOW_REACH, kvw), BF),
            pltpu.VMEM((length + 32, chans), F32),
            pltpu.VMEM((length, chans), F32),
            pltpu.VMEM((4, 8, length), F32),
            pltpu.VMEM((length, chans + qwidth), BF),
            pltpu.VMEM((length, ob), F32),
            pltpu.VMEM((n, 2 * tl, ob), BF),
            pltpu.VMEM((n, 2 * tl, ob), BF),
            pltpu.VMEM((n, tl, ob), BF),
            pltpu.VMEM((n, tl, ob), BF),
            pltpu.VMEM((n, 2 * tl, ob), F32),
            dma((7,)),
            dma((3, 2)),
            dma((3, 2)),
            dma((3, 2, half, 2)),
            dma((3, 2, half, 2)),
            dma((4,)),
            dma((4,)),
            dma((3,)),
            dma((3,)),
            dma((n,)),
            dma((n,)),
            dma((n,)),
            dma((n,)),
        ],
        compiler_params=pltpu.CompilerParams(
            collective_id=0, has_side_effects=True, vmem_limit_bytes=56 * 1024 * 1024
        ),
    )(
        tokens, in_gain.reshape(1, width), w_conv_val, w_conv_gate, w_query, wkv, conv_taps,
        conv_bias.reshape(1, chans), norm_gain.reshape(1, chans), norm_bias.reshape(1, chans),
        head_sink_logit.reshape(1, heads), w_out_conv, w_out_attn,
    )


def solution(mesh):
    return jax.shard_map(
        functools.partial(layer, mesh.shape["sp"], mesh.shape["tp"]),
        mesh=mesh,
        in_specs=(
            P(("sp", "tp"), None),
            P(),
            P("sp", "tp"),
            P("sp", "tp"),
            P("sp", "tp"),
            P("sp", "tp"),
            P("sp", "tp"),
            P(None, "tp"),
            P("tp"),
            P("tp"),
            P("tp"),
            P("tp"),
            P("tp", "sp"),
            P("tp", "sp"),
        ),
        out_specs=(P(("sp", "tp"), None), P("sp", "tp")),
        check_vma=False,
    )
```

```python
import functools

import jax
import jax.numpy as jnp
from jax import lax
from jax.experimental import pallas as pl
from jax.experimental.pallas import tpu as pltpu
from jax.sharding import PartitionSpec as P

WINDOW_REACH = 128


def with_halo(cells, sides, width):
    for axis, dim in sides:
        count = lax.axis_size(axis)
        ends = count - 1
        head = lax.slice_in_dim(cells, 0, width, axis=dim)
        tail = lax.slice_in_dim(cells, cells.shape[dim] - width, cells.shape[dim], axis=dim)
        cells = jnp.concatenate(
            [
                lax.ppermute(tail, axis, [(i, (i + 1) % count) for i in range(ends)]),
                cells,
                lax.ppermute(head, axis, [((i + 1) % count, i) for i in range(ends)]),
            ],
            axis=dim,
        )
    return cells


def on_device(
    tokens,
    in_gain,
    w_conv_val,
    w_conv_gate,
    w_query,
    w_key,
    value_weight,
    conv_taps,
    conv_bias,
    norm_gain,
    norm_bias,
    head_sink_logit,
    w_out_conv,
    w_out_attn,
):
    flt = tokens.astype(jnp.float32)
    normed = (
        flt * lax.rsqrt(jnp.mean(flt * flt, axis=-1, keepdims=True) + 1e-06) * in_gain
    ).astype(jnp.bfloat16)
    val_full, gate_full, query_full, key_full, value_full = (
        lax.all_gather(w_conv_val, "sp", axis=0, tiled=True),
        lax.all_gather(w_conv_gate, "sp", axis=0, tiled=True),
        lax.all_gather(w_query, "sp", axis=0, tiled=True),
        lax.all_gather(w_key, "sp", axis=0, tiled=True),
        lax.all_gather(value_weight, "sp", axis=0, tiled=True),
    )
    joined = jnp.concatenate([val_full, gate_full, query_full, key_full, value_full], axis=1)
    projected = jnp.dot(
        lax.all_gather(normed, "tp", axis=0, tiled=True), joined, preferred_element_type=jnp.float32
    )
    chans = val_full.shape[1]
    qwidth = query_full.shape[1]
    kwidth = key_full.shape[1]
    length = projected.shape[0]
    glu = (projected[:, :chans] * jax.nn.sigmoid(projected[:, chans : 2 * chans])).astype(
        jnp.bfloat16
    )
    base = 2 * chans
    query_matrix = projected[:, base : base + qwidth].astype(jnp.bfloat16)
    key = projected[:, base + qwidth : base + qwidth + kwidth].astype(jnp.bfloat16)
    value_matrix = projected[:, base + qwidth + kwidth :].astype(jnp.bfloat16)
    taps = conv_taps.shape[0]
    half = taps // 2
    padded = with_halo(glu, (("sp", 0),), half)
    filtered = jnp.zeros(glu.shape, jnp.float32) + conv_bias
    for offset in range(taps):
        filtered = (
            filtered + padded[offset : offset + length].astype(jnp.float32) * conv_taps[offset]
        )
    sums, squares = lax.psum(
        (jnp.sum(filtered, axis=-1), jnp.sum(filtered * filtered, axis=-1)), "tp"
    )
    count = chans * lax.axis_size("tp")
    center = (sums / count)[:, None]
    spread = (squares / count)[:, None] - center * center
    conv_out = jax.nn.silu(
        (filtered - center) * lax.rsqrt(spread + 1e-05) * norm_gain + norm_bias
    ).astype(jnp.bfloat16)
    heads_here = head_sink_logit.shape[0]
    head_size = qwidth // heads_here
    kv_here = kwidth // head_size
    query_groups = heads_here // kv_here
    stacked = jnp.stack([key, value_matrix], axis=0)
    banded = with_halo(stacked, (("sp", 1),), WINDOW_REACH)
    span = length + 2 * WINDOW_REACH
    key_band = banded[0].reshape(span, kv_here, head_size)
    value_band = banded[1].reshape(span, kv_here, head_size)
    query4_grouped = query_matrix.reshape(length, kv_here, query_groups, head_size)
    scores = jnp.einsum(
        "qkgd,jkd->kgqj", query4_grouped, key_band, preferred_element_type=jnp.float32
    ) * head_size ** (-0.5)
    offset_pos = lax.axis_index("sp") * length
    seq_len = length * lax.axis_size("sp")
    qpos = offset_pos + jnp.arange(length, dtype=jnp.int32)
    kpos = offset_pos - WINDOW_REACH + jnp.arange(span, dtype=jnp.int32)
    valid = (
        (jnp.abs(qpos[:, None] - kpos[None, :]) <= WINDOW_REACH)
        & (kpos[None, :] >= 0)
        & (kpos[None, :] < seq_len)
    )
    sink_column = head_sink_logit.reshape(kv_here, query_groups, 1)
    masked = jnp.where(valid, scores, -1e30)
    top = jnp.maximum(jnp.max(masked, axis=-1), sink_column)
    expd = jnp.where(valid, jnp.exp(masked - top[..., None]), 0.0)
    total = jnp.sum(expd, axis=-1) + jnp.exp(sink_column - top)
    probs = (expd / total[..., None]).astype(jnp.bfloat16)
    attended = jnp.einsum(
        "kgqj,jkd->qkgd", probs, value_band, preferred_element_type=jnp.float32
    ).astype(jnp.bfloat16)
    attended = attended.reshape(length, qwidth)
    log_total = (top + jnp.log(total)).reshape(heads_here, length).T
    out_conv_cols, out_attn_cols = (
        lax.all_gather(w_out_conv, "sp", axis=1, tiled=True),
        lax.all_gather(w_out_attn, "sp", axis=1, tiled=True),
    )
    out_rows = jnp.concatenate([out_conv_cols, out_attn_cols], axis=0)
    features = jnp.concatenate([conv_out, attended], axis=1)
    mixed = lax.psum_scatter(
        jnp.dot(features, out_rows, preferred_element_type=jnp.float32).astype(jnp.bfloat16),
        "tp",
        scatter_dimension=0,
        tiled=True,
    )
    return (mixed, log_total)


BF = jnp.bfloat16
F32 = jnp.float32


def fused_kernel(
    n, x_hbm, gain, wval, wgate, wquery, wkey, wvalue, taps, cbias, ngain, nbias, sink, woc, woa,
    mixed, logt,
    tok, nrm, wq, wc, wo, accq, accc, qb, band, glu, filt, stat, feat, part,
    p1s, p1r, p2s, p2r, own,
    lsem, tsem, trec, rsem, rrec, hsem, hrec, ssem, srec, asem, arec, bsem, brec,
):
    sp = lax.axis_index("sp")
    t = lax.axis_index("tp")
    half = n // 2
    tl, width = x_hbm.shape
    length = 4 * tl
    kb = wval.shape[0]
    chans = wval.shape[1]
    qwidth = wquery.shape[1]
    hd = wkey.shape[0]
    kvw = 2 * hd
    heads = sink.shape[1]
    ob = woc.shape[1]
    reach = WINDOW_REACH
    y, c = t // 2, t % 2
    core_peer = y * 2 + 1 - c
    y_peer = (1 - y) * 2 + c
    far_peer = (1 - y) * 2 + 1 - c
    xbit, zpos = sp % 2, sp // 2
    pos = (1 - xbit) * zpos + xbit * (n - 1 - zpos)

    def at_pos(q):
        q = (q + 2 * n) % n
        hi = q // half
        return (1 - hi) * (2 * q) + hi * (2 * (n - 1 - q) + 1)

    right, left = at_pos(pos + 1), at_pos(pos - 1)
    nxt, prv = (sp + 1) % n, (sp + n - 1) % n

    def rows(o, size):
        return pl.ds(pl.multiple_of(o * size, size), size)

    local = [
        pltpu.make_async_copy(x_hbm, tok.at[rows(t, tl)], lsem.at[0]),
        pltpu.make_async_copy(wquery, wq.at[sp, pl.ds(0, kb)], lsem.at[1]),
        pltpu.make_async_copy(wkey, wq.at[sp, pl.ds(kb, hd)], lsem.at[2]),
        pltpu.make_async_copy(wvalue, wq.at[sp, pl.ds(kb + hd, hd)], lsem.at[7]),
        pltpu.make_async_copy(wval, wc.at[rows(sp, kb), pl.ds(0, chans)], lsem.at[3]),
        pltpu.make_async_copy(wgate, wc.at[rows(sp, kb), pl.ds(chans, chans)], lsem.at[4]),
        pltpu.make_async_copy(woc, wo.at[sp, pl.ds(0, chans)], lsem.at[5]),
        pltpu.make_async_copy(woa, wo.at[sp, pl.ds(chans, qwidth)], lsem.at[6]),
    ]
    for cp in local:
        cp.start()
    barrier = pltpu.get_barrier_semaphore()
    for dev in (right, left, nxt, prv):
        pl.semaphore_signal(
            barrier, inc=1, device_id={"sp": dev}, device_id_type=pl.DeviceIdType.MESH
        )
    for dev in (core_peer, y_peer, far_peer):
        pl.semaphore_signal(
            barrier, inc=1, device_id={"tp": dev}, device_id_type=pl.DeviceIdType.MESH
        )
    pl.semaphore_wait(barrier, 7)

    sent = []

    def remote(src, dst, ss, rs, dev):
        cp = pltpu.make_async_remote_copy(
            src_ref=src, dst_ref=dst, send_sem=ss, recv_sem=rs, device_id=dev,
            device_id_type=pl.DeviceIdType.MESH,
        )
        cp.start()
        sent.append(cp)
        return cp

    ring = {}

    def block_ref(k, o, h):
        if k == 0:
            depth = wq.shape[1] // 2
            return wq.at[o, pl.ds(h * depth, depth)]
        if k == 1:
            return wc.at[pl.ds(pl.multiple_of(o * kb + h * (kb // 2), kb // 2), kb // 2)]
        depth = wo.shape[1] // 2
        return wo.at[o, pl.ds(h * depth, depth)]

    def ring_event(k, s, halves=(0, 1)):
        for h in halves:
            for d in (0, 1):
                if s > 1:
                    ring[k, d, s - 1, h].wait_recv()
                if s < half or h == d:
                    o = at_pos(pos - (s - 1) if d == 0 else pos + (s - 1))
                    ref = block_ref(k, o, h)
                    ring[k, d, s, h] = remote(
                        ref, ref, rsem.at[k, d, s - 1, h], rrec.at[k, d, s - 1, h],
                        {"sp": right if d == 0 else left},
                    )

    def ring_last(k):
        for d in (0, 1):
            ring[k, d, half, d].wait_recv()

    def owners(s):
        if s == 0:
            return [sp]
        if s == half:
            return [at_pos(pos + half)]
        return [at_pos(pos - s), at_pos(pos + s)]

    local[4].wait()
    local[5].wait()
    ring_event(1, 1)
    local[0].wait()
    hl = tl // 2
    tokcp = {}

    def tok_send(slot, h, e, dev):
        ref = tok.at[pl.ds(pl.multiple_of(slot * tl + h * hl, hl), hl)]
        tokcp[e, h] = remote(ref, ref, tsem.at[e, h], trec.at[e, h], {"tp": dev})

    for h in (0, 1):
        tok_send(t, h, 0, y_peer)
    for h in (0, 1):
        tok_send(t, h, 1, core_peer)
    for i in (1, 2, 3, 6, 7):
        local[i].wait()

    def norm_rows(slot):
        step = 32

        def body(i, carry):
            r = pl.ds(pl.multiple_of(slot * tl + i * step, step), step)
            flt = tok[r, :].astype(F32)
            scale = lax.rsqrt(jnp.mean(flt * flt, axis=-1, keepdims=True) + 1e-06)
            nrm[r, :] = (flt * scale * gain[...]).astype(BF)
            return carry

        lax.fori_loop(0, tl // step, body, 0)

    norm_rows(t)
    for h in (0, 1):
        tokcp[1, h].wait_recv()
    ring_event(1, 2, (0,))
    norm_rows(core_peer)
    ring_event(1, 2, (1,))
    tokcp[0, 0].wait_recv()
    tok_send(y_peer, 0, 2, core_peer)
    ring_event(1, 3, (0,))
    ring_event(1, 3, (1,))
    tokcp[0, 1].wait_recv()
    tok_send(y_peer, 1, 2, core_peer)
    ring_event(0, 1, (0,))
    norm_rows(y_peer)
    for h in (0, 1):
        tokcp[2, h].wait_recv()
    norm_rows(far_peer)

    def columns(o):
        return nrm[:, pl.ds(pl.multiple_of(o * kb, kb), kb)]

    def project_conv(s):
        for o in owners(s):
            res = jnp.dot(columns(o), wc[rows(o, kb), :], preferred_element_type=F32)
            accc[...] = res if s == 0 else accc[...] + res

    def project_heads(s):
        for o in owners(s):
            lhs = columns(o)
            res = jnp.dot(lhs, wq[o, 0:kb, :], preferred_element_type=F32)
            two = lax.dot_general(
                lhs, wq[o, kb : kb + kvw, :], (((1,), (1,)), ((), ())),
                preferred_element_type=F32,
            )
            if s == 0:
                accq[:, 0:qwidth] = res
                accq[:, qwidth : qwidth + kvw] = two
            else:
                accq[:, 0:qwidth] = accq[:, 0:qwidth] + res
                accq[:, qwidth : qwidth + kvw] = accq[:, qwidth : qwidth + kvw] + two

    project_conv(0)
    ring_event(1, 4)
    ring_event(0, 1, (1,))
    project_conv(1)
    project_conv(2)
    project_conv(3)
    ring_event(0, 2, (0,))
    ring_last(1)
    project_conv(4)
    pad = 16
    glu[pl.ds(pad, length), :] = (
        (accc[:, 0:chans] * jax.nn.sigmoid(accc[:, chans : 2 * chans])).astype(BF).astype(F32)
    )
    g_up = remote(
        glu.at[pl.ds(length, pad)], glu.at[pl.ds(0, pad)], hsem.at[2], hrec.at[2], {"sp": nxt}
    )
    g_down = remote(
        glu.at[pl.ds(pad, pad)], glu.at[pl.ds(length + pad, pad)], hsem.at[3], hrec.at[3],
        {"sp": prv},
    )
    ring_event(0, 2, (1,))
    ntaps = taps.shape[0]
    off = pad - ntaps // 2
    cstep = 64

    def conv_rows(r0):
        acc = jnp.zeros((cstep, chans), F32) + cbias[...]
        for j in range(ntaps):
            acc = acc + glu[pl.ds(r0 + off + j, cstep), :] * taps[pl.ds(j, 1), :]
        filt[pl.ds(r0, cstep), :] = acc

    nconv = length // cstep
    for i in range(1, nconv - 1):
        conv_rows(i * cstep)
    ring_event(0, 3)
    g_up.wait_recv()
    g_down.wait_recv()

    @pl.when(sp == 0)
    def _():
        glu[pl.ds(0, pad), :] = jnp.zeros((pad, chans), F32)

    @pl.when(sp == n - 1)
    def _():
        glu[pl.ds(length + pad, pad), :] = jnp.zeros((pad, chans), F32)

    conv_rows(0)
    conv_rows((nconv - 1) * cstep)
    lane = lax.broadcasted_iota(jnp.int32, (128, 128), 1)
    for b in range(length // 128):
        f = filt[pl.ds(b * 128, 128), :]
        s1 = jnp.sum(f, axis=-1, keepdims=True)
        s2 = jnp.sum(f * f, axis=-1, keepdims=True)
        tile = jnp.where(lane == 0, s1, jnp.where(lane == 1, s2, 0.0))
        stat[pl.ds(t, 1), :, pl.ds(b * 128, 128)] = jnp.transpose(tile)[None, 0:8, :]
    scp = []
    for e, dev in enumerate((y_peer, far_peer, core_peer)):
        scp.append(remote(stat.at[t], stat.at[t], ssem.at[e], srec.at[e], {"tp": dev}))
    ring_event(2, 1, (0,))
    ring_event(0, 4)
    ring_event(2, 1, (1,))
    project_heads(0)
    project_heads(1)
    project_heads(2)
    for cp in scp:
        cp.wait_recv()
    count = chans * 4
    for b in range(length // 128):
        cols = pl.ds(b * 128, 128)
        tot = (stat[0, :, cols] + stat[1, :, cols] + stat[2, :, cols] + stat[3, :, cols]) / count
        tt = jnp.transpose(jnp.concatenate([tot] * 16, axis=0))
        center = tt[:, 0:1]
        spread = tt[:, 1:2] - center * center
        u = (filt[pl.ds(b * 128, 128), :] - center) * lax.rsqrt(spread + 1e-05)
        u = u * ngain[...] + nbias[...]
        feat[pl.ds(b * 128, 128), 0:chans] = (u * jax.nn.sigmoid(u)).astype(BF)

    project_heads(3)
    ring_last(0)
    project_heads(4)
    qb[...] = accq[:, 0:qwidth].astype(BF)
    band[pl.ds(reach, length), :] = accq[:, qwidth : qwidth + kvw].astype(BF)
    kv_up = remote(
        band.at[pl.ds(length, reach)], band.at[pl.ds(0, reach)], hsem.at[0], hrec.at[0],
        {"sp": nxt},
    )
    kv_down = remote(
        band.at[pl.ds(reach, reach)], band.at[pl.ds(length + reach, reach)], hsem.at[1],
        hrec.at[1], {"sp": prv},
    )
    seq_len = length * n

    def attend(b):
        blk = reach
        span = blk + 2 * reach
        kk = band[pl.ds(b * blk, span), 0:hd]
        vv = band[pl.ds(b * blk, span), hd:kvw]
        ri = lax.broadcasted_iota(jnp.int32, (blk, span), 0)
        ci = lax.broadcasted_iota(jnp.int32, (blk, span), 1)
        kp = sp * length + b * blk - reach + ci
        valid = (ci >= ri) & (ci <= ri + 2 * reach) & (kp >= 0) & (kp < seq_len)
        logs = []
        for h in range(heads):
            q = qb[pl.ds(b * blk, blk), h * hd : (h + 1) * hd]
            s = lax.dot_general(
                q, kk, (((1,), (1,)), ((), ())), preferred_element_type=F32
            ) * hd ** (-0.5)
            s = jnp.where(valid, s, -1e30)
            sk = sink[0:1, h : h + 1]
            top = jnp.maximum(jnp.max(s, axis=-1, keepdims=True), sk)
            e = jnp.where(valid, jnp.exp(s - top), 0.0)
            total = jnp.sum(e, axis=-1, keepdims=True) + jnp.exp(sk - top)
            p = (e * (1.0 / total)).astype(BF)
            a = jnp.dot(p, vv, preferred_element_type=F32).astype(BF)
            feat[pl.ds(b * blk, blk), chans + h * hd : chans + (h + 1) * hd] = a
            logs.append(top + jnp.log(total))
        wide = jnp.zeros((blk, 128), F32)
        for h in range(heads):
            wide = jnp.where(lane == h, logs[h], wide)
        logt[:, pl.ds(b * blk, blk)] = jnp.transpose(wide)[0:heads, :]

    nblk = length // reach
    for b in range(1, nblk - 1):
        attend(b)
    ring_event(2, 2)
    kv_up.wait_recv()
    kv_down.wait_recv()
    attend(0)
    attend(nblk - 1)

    acp, bcp = {}, {}
    order = []

    def emit(o):
        i = len(order)
        order.append(o)
        part[...] = jnp.dot(feat[...], wo[o], preferred_element_type=F32)
        p1s[i, pl.ds(0, tl), :] = part[rows(core_peer, tl), :].astype(BF)
        p1s[i, pl.ds(tl, tl), :] = part[rows(far_peer, tl), :].astype(BF)
        acp[i] = remote(p1s.at[i], p1r.at[i], asem.at[i], arec.at[i], {"tp": core_peer})
        own[i, pl.ds(0, tl), :] = part[rows(t, tl), :]
        own[i, pl.ds(tl, tl), :] = part[rows(y_peer, tl), :]

    def cross(i):
        acp[i].wait_recv()
        p2s[i] = (own[i, pl.ds(tl, tl), :] + p1r[i, pl.ds(tl, tl), :].astype(F32)).astype(BF)
        bcp[i] = remote(p2s.at[i], p2r.at[i], bsem.at[i], brec.at[i], {"tp": y_peer})

    def finish(i):
        bcp[i].wait_recv()
        mixed[:, rows(order[i], ob)] = (
            own[i, pl.ds(0, tl), :] + p1r[i, pl.ds(0, tl), :].astype(F32)
            + p2r[i].astype(F32)
        ).astype(BF)

    def out_step(s):
        for o in owners(s):
            emit(o)
            if len(order) >= 2:
                cross(len(order) - 2)

    out_step(0)
    ring_event(2, 3)
    out_step(1)
    out_step(2)
    ring_event(2, 4)
    out_step(3)
    for i in range(n - 4):
        finish(i)
    ring_last(2)
    out_step(half)
    for i in range(n - 4, n - 2):
        finish(i)
    cross(n - 1)
    finish(n - 2)
    finish(n - 1)
    for cp in sent:
        cp.wait_send()


def layer(
    n, parts, tokens, in_gain, w_conv_val, w_conv_gate, w_query, w_key, value_weight, conv_taps,
    conv_bias, norm_gain, norm_bias, head_sink_logit, w_out_conv, w_out_attn,
):
    tl, width = tokens.shape
    kb, chans = w_conv_val.shape
    qwidth = w_query.shape[1]
    kvw = 2 * w_key.shape[1]
    heads = head_sink_logit.shape[0]
    ob = w_out_conv.shape[1]
    fits = (
        parts == 4 and n == 8 and tl % 128 == 0 and kb % 128 == 0 and ob % 128 == 0
        and chans % 128 == 0 and kvw == 128 and kb == qwidth and qwidth == heads * kvw // 2
        and conv_taps.shape[0] <= 33
    )
    if not fits:
        return on_device(
            tokens, in_gain, w_conv_val, w_conv_gate, w_query, w_key, value_weight, conv_taps,
            conv_bias, norm_gain, norm_bias, head_sink_logit, w_out_conv, w_out_attn,
        )
    length = 4 * tl
    half = n // 2
    vm = pl.BlockSpec(memory_space=pltpu.VMEM)
    hb = pl.BlockSpec(memory_space=pl.ANY)
    dma = pltpu.SemaphoreType.DMA
    mixed, log_rows = pl.pallas_call(
        functools.partial(fused_kernel, n),
        out_shape=(
            jax.ShapeDtypeStruct((tl, width), BF),
            jax.ShapeDtypeStruct((heads, length), F32),
        ),
        in_specs=[hb, vm, hb, hb, hb, hb, hb, vm, vm, vm, vm, vm, hb, hb],
        out_specs=(vm, vm),
        scratch_shapes=[
            pltpu.VMEM((length, width), BF),
            pltpu.VMEM((length, width), BF),
            pltpu.VMEM((n, kb + kvw, qwidth), BF),
            pltpu.VMEM((n * kb, 2 * chans), BF),
            pltpu.VMEM((n, chans + qwidth, ob), BF),
            pltpu.VMEM((length, qwidth + kvw), F32),
            pltpu.VMEM((length, 2 * chans), F32),
            pltpu.VMEM((length, qwidth), BF),
            pltpu.VMEM((length + 2 * WINDOW_REACH, kvw), BF),
            pltpu.VMEM((length + 32, chans), F32),
            pltpu.VMEM((length, chans), F32),
            pltpu.VMEM((4, 8, length), F32),
            pltpu.VMEM((length, chans + qwidth), BF),
            pltpu.VMEM((length, ob), F32),
            pltpu.VMEM((n, 2 * tl, ob), BF),
            pltpu.VMEM((n, 2 * tl, ob), BF),
            pltpu.VMEM((n, tl, ob), BF),
            pltpu.VMEM((n, tl, ob), BF),
            pltpu.VMEM((n, 2 * tl, ob), F32),
            dma((8,)),
            dma((3, 2)),
            dma((3, 2)),
            dma((3, 2, half, 2)),
            dma((3, 2, half, 2)),
            dma((4,)),
            dma((4,)),
            dma((3,)),
            dma((3,)),
            dma((n,)),
            dma((n,)),
            dma((n,)),
            dma((n,)),
        ],
        compiler_params=pltpu.CompilerParams(
            collective_id=0, has_side_effects=True, vmem_limit_bytes=56 * 1024 * 1024
        ),
    )(
        tokens, in_gain.reshape(1, width), w_conv_val, w_conv_gate, w_query, w_key.T, value_weight.T,
        conv_taps, conv_bias.reshape(1, chans), norm_gain.reshape(1, chans), norm_bias.reshape(1, chans),
        head_sink_logit.reshape(1, heads), w_out_conv, w_out_attn,
    )
    return mixed, log_rows.T


def solution(mesh):
    return jax.shard_map(
        functools.partial(layer, mesh.shape["sp"], mesh.shape["tp"]),
        mesh=mesh,
        in_specs=(
            P(("sp", "tp"), None),
            P(),
            P("sp", "tp"),
            P("sp", "tp"),
            P("sp", "tp"),
            P("sp", "tp"),
            P("sp", "tp"),
            P(None, "tp"),
            P("tp"),
            P("tp"),
            P("tp"),
            P("tp"),
            P("tp", "sp"),
            P("tp", "sp"),
        ),
        out_specs=(P(("sp", "tp"), None), P("sp", "tp")),
        check_vma=False,
    )
```

```python
import functools

import jax
import jax.numpy as jnp
from jax import lax
from jax.experimental import pallas as pl
from jax.experimental.pallas import tpu as pltpu
from jax.sharding import PartitionSpec as P

WINDOW_REACH = 128


def with_halo(cells, sides, width):
    for axis, dim in sides:
        count = lax.axis_size(axis)
        ends = count - 1
        head = lax.slice_in_dim(cells, 0, width, axis=dim)
        tail = lax.slice_in_dim(cells, cells.shape[dim] - width, cells.shape[dim], axis=dim)
        cells = jnp.concatenate(
            [
                lax.ppermute(tail, axis, [(i, (i + 1) % count) for i in range(ends)]),
                cells,
                lax.ppermute(head, axis, [((i + 1) % count, i) for i in range(ends)]),
            ],
            axis=dim,
        )
    return cells


def on_device(
    tokens,
    in_gain,
    w_conv_val,
    w_conv_gate,
    w_query,
    w_key,
    value_weight,
    conv_taps,
    conv_bias,
    norm_gain,
    norm_bias,
    head_sink_logit,
    w_out_conv,
    w_out_attn,
):
    flt = tokens.astype(jnp.float32)
    normed = (
        flt * lax.rsqrt(jnp.mean(flt * flt, axis=-1, keepdims=True) + 1e-06) * in_gain
    ).astype(jnp.bfloat16)
    val_full, gate_full, query_full, key_full, value_full = (
        lax.all_gather(w_conv_val, "sp", axis=0, tiled=True),
        lax.all_gather(w_conv_gate, "sp", axis=0, tiled=True),
        lax.all_gather(w_query, "sp", axis=0, tiled=True),
        lax.all_gather(w_key, "sp", axis=0, tiled=True),
        lax.all_gather(value_weight, "sp", axis=0, tiled=True),
    )
    joined = jnp.concatenate([val_full, gate_full, query_full, key_full, value_full], axis=1)
    projected = jnp.dot(
        lax.all_gather(normed, "tp", axis=0, tiled=True), joined, preferred_element_type=jnp.float32
    )
    chans = val_full.shape[1]
    qwidth = query_full.shape[1]
    kwidth = key_full.shape[1]
    length = projected.shape[0]
    glu = (projected[:, :chans] * jax.nn.sigmoid(projected[:, chans : 2 * chans])).astype(
        jnp.bfloat16
    )
    base = 2 * chans
    query_matrix = projected[:, base : base + qwidth].astype(jnp.bfloat16)
    key = projected[:, base + qwidth : base + qwidth + kwidth].astype(jnp.bfloat16)
    value_matrix = projected[:, base + qwidth + kwidth :].astype(jnp.bfloat16)
    taps = conv_taps.shape[0]
    half = taps // 2
    padded = with_halo(glu, (("sp", 0),), half)
    filtered = jnp.zeros(glu.shape, jnp.float32) + conv_bias
    for offset in range(taps):
        filtered = (
            filtered + padded[offset : offset + length].astype(jnp.float32) * conv_taps[offset]
        )
    sums, squares = lax.psum(
        (jnp.sum(filtered, axis=-1), jnp.sum(filtered * filtered, axis=-1)), "tp"
    )
    count = chans * lax.axis_size("tp")
    center = (sums / count)[:, None]
    spread = (squares / count)[:, None] - center * center
    conv_out = jax.nn.silu(
        (filtered - center) * lax.rsqrt(spread + 1e-05) * norm_gain + norm_bias
    ).astype(jnp.bfloat16)
    heads_here = head_sink_logit.shape[0]
    head_size = qwidth // heads_here
    kv_here = kwidth // head_size
    query_groups = heads_here // kv_here
    stacked = jnp.stack([key, value_matrix], axis=0)
    banded = with_halo(stacked, (("sp", 1),), WINDOW_REACH)
    span = length + 2 * WINDOW_REACH
    key_band = banded[0].reshape(span, kv_here, head_size)
    value_band = banded[1].reshape(span, kv_here, head_size)
    query4_grouped = query_matrix.reshape(length, kv_here, query_groups, head_size)
    scores = jnp.einsum(
        "qkgd,jkd->kgqj", query4_grouped, key_band, preferred_element_type=jnp.float32
    ) * head_size ** (-0.5)
    offset_pos = lax.axis_index("sp") * length
    seq_len = length * lax.axis_size("sp")
    qpos = offset_pos + jnp.arange(length, dtype=jnp.int32)
    kpos = offset_pos - WINDOW_REACH + jnp.arange(span, dtype=jnp.int32)
    valid = (
        (jnp.abs(qpos[:, None] - kpos[None, :]) <= WINDOW_REACH)
        & (kpos[None, :] >= 0)
        & (kpos[None, :] < seq_len)
    )
    sink_column = head_sink_logit.reshape(kv_here, query_groups, 1)
    masked = jnp.where(valid, scores, -1e30)
    top = jnp.maximum(jnp.max(masked, axis=-1), sink_column)
    expd = jnp.where(valid, jnp.exp(masked - top[..., None]), 0.0)
    total = jnp.sum(expd, axis=-1) + jnp.exp(sink_column - top)
    probs = (expd / total[..., None]).astype(jnp.bfloat16)
    attended = jnp.einsum(
        "kgqj,jkd->qkgd", probs, value_band, preferred_element_type=jnp.float32
    ).astype(jnp.bfloat16)
    attended = attended.reshape(length, qwidth)
    log_total = (top + jnp.log(total)).reshape(heads_here, length).T
    out_conv_cols, out_attn_cols = (
        lax.all_gather(w_out_conv, "sp", axis=1, tiled=True),
        lax.all_gather(w_out_attn, "sp", axis=1, tiled=True),
    )
    out_rows = jnp.concatenate([out_conv_cols, out_attn_cols], axis=0)
    features = jnp.concatenate([conv_out, attended], axis=1)
    mixed = lax.psum_scatter(
        jnp.dot(features, out_rows, preferred_element_type=jnp.float32).astype(jnp.bfloat16),
        "tp",
        scatter_dimension=0,
        tiled=True,
    )
    return (mixed, log_total)


BF = jnp.bfloat16
F32 = jnp.float32


def fused_kernel(
    n, x_hbm, gain, wval, wgate, wquery, wkey, wvalue, taps, cbias, ngain, nbias, sink, woc, woa,
    mixed, logt,
    tok, nrm, wq, wc, wo, accq, accc, qb, band, glu, filt, stat, feat, part,
    p1s, p1r, p2s, p2r, own,
    lsem, tsem, trec, rsem, rrec, hsem, hrec, ssem, srec, asem, arec, bsem, brec,
):
    sp = lax.axis_index("sp")
    t = lax.axis_index("tp")
    half = n // 2
    tl, width = x_hbm.shape
    length = 4 * tl
    kb = wval.shape[0]
    chans = wval.shape[1]
    qwidth = wquery.shape[1]
    hd = wkey.shape[0]
    kvw = 2 * hd
    heads = sink.shape[1]
    ob = woc.shape[1]
    reach = WINDOW_REACH
    y, c = t // 2, t % 2
    core_peer = y * 2 + 1 - c
    y_peer = (1 - y) * 2 + c
    far_peer = (1 - y) * 2 + 1 - c
    xbit, zpos = sp % 2, sp // 2
    pos = (1 - xbit) * zpos + xbit * (n - 1 - zpos)

    def at_pos(q):
        q = (q + 2 * n) % n
        hi = q // half
        return (1 - hi) * (2 * q) + hi * (2 * (n - 1 - q) + 1)

    right, left = at_pos(pos + 1), at_pos(pos - 1)
    nxt, prv = (sp + 1) % n, (sp + n - 1) % n

    def rows(o, size):
        return pl.ds(pl.multiple_of(o * size, size), size)

    local = [
        pltpu.make_async_copy(x_hbm, tok.at[rows(t, tl)], lsem.at[0]),
        pltpu.make_async_copy(wquery, wq.at[sp, pl.ds(0, kb)], lsem.at[1]),
        pltpu.make_async_copy(wkey, wq.at[sp, pl.ds(kb, hd)], lsem.at[2]),
        pltpu.make_async_copy(wvalue, wq.at[sp, pl.ds(kb + hd, hd)], lsem.at[7]),
        pltpu.make_async_copy(wval, wc.at[rows(sp, kb), pl.ds(0, chans)], lsem.at[3]),
        pltpu.make_async_copy(wgate, wc.at[rows(sp, kb), pl.ds(chans, chans)], lsem.at[4]),
        pltpu.make_async_copy(woc, wo.at[sp, pl.ds(0, chans)], lsem.at[5]),
        pltpu.make_async_copy(woa, wo.at[sp, pl.ds(chans, qwidth)], lsem.at[6]),
    ]
    for cp in local:
        cp.start()
    barrier = pltpu.get_barrier_semaphore()
    for dev in (right, left, nxt, prv):
        pl.semaphore_signal(
            barrier, inc=1, device_id={"sp": dev}, device_id_type=pl.DeviceIdType.MESH
        )
    for dev in (core_peer, y_peer, far_peer):
        pl.semaphore_signal(
            barrier, inc=1, device_id={"tp": dev}, device_id_type=pl.DeviceIdType.MESH
        )
    pl.semaphore_wait(barrier, 7)

    sent = []

    def remote(src, dst, ss, rs, dev):
        cp = pltpu.make_async_remote_copy(
            src_ref=src, dst_ref=dst, send_sem=ss, recv_sem=rs, device_id=dev,
            device_id_type=pl.DeviceIdType.MESH,
        )
        cp.start()
        sent.append(cp)
        return cp

    ring = {}

    def block_ref(k, o, h):
        if k == 0:
            depth = wq.shape[1] // 2
            return wq.at[o, pl.ds(h * depth, depth)]
        if k == 1:
            return wc.at[pl.ds(pl.multiple_of(o * kb + h * (kb // 2), kb // 2), kb // 2)]
        depth = wo.shape[1] // 2
        return wo.at[o, pl.ds(h * depth, depth)]

    def ring_event(k, s, halves=(0, 1)):
        for h in halves:
            for d in (0, 1):
                if s > 1:
                    ring[k, d, s - 1, h].wait_recv()
                if s < half or h == d:
                    o = at_pos(pos - (s - 1) if d == 0 else pos + (s - 1))
                    ref = block_ref(k, o, h)
                    ring[k, d, s, h] = remote(
                        ref, ref, rsem.at[k, d, s - 1, h], rrec.at[k, d, s - 1, h],
                        {"sp": right if d == 0 else left},
                    )

    def ring_last(k):
        for d in (0, 1):
            ring[k, d, half, d].wait_recv()

    def owners(s):
        if s == 0:
            return [sp]
        if s == half:
            return [at_pos(pos + half)]
        return [at_pos(pos - s), at_pos(pos + s)]

    local[4].wait()
    local[5].wait()
    ring_event(1, 1)
    local[0].wait()
    hl = tl // 2
    tokcp = {}

    def tok_send(slot, h, e, dev):
        ref = tok.at[pl.ds(pl.multiple_of(slot * tl + h * hl, hl), hl)]
        tokcp[e, h] = remote(ref, ref, tsem.at[e, h], trec.at[e, h], {"tp": dev})

    for h in (0, 1):
        tok_send(t, h, 0, y_peer)
    for h in (0, 1):
        tok_send(t, h, 1, core_peer)
    for i in (1, 2, 3, 6, 7):
        local[i].wait()

    def norm_rows(slot):
        step = 32

        def body(i, carry):
            r = pl.ds(pl.multiple_of(slot * tl + i * step, step), step)
            flt = tok[r, :].astype(F32)
            scale = lax.rsqrt(jnp.mean(flt * flt, axis=-1, keepdims=True) + 1e-06)
            nrm[r, :] = (flt * scale * gain[...]).astype(BF)
            return carry

        lax.fori_loop(0, tl // step, body, 0)

    norm_rows(t)
    for h in (0, 1):
        tokcp[1, h].wait_recv()
    ring_event(1, 2, (0,))
    norm_rows(core_peer)
    ring_event(1, 2, (1,))
    tokcp[0, 0].wait_recv()
    tok_send(y_peer, 0, 2, core_peer)
    ring_event(1, 3, (0,))
    ring_event(1, 3, (1,))
    tokcp[0, 1].wait_recv()
    tok_send(y_peer, 1, 2, core_peer)
    ring_event(0, 1, (0,))
    norm_rows(y_peer)
    for h in (0, 1):
        tokcp[2, h].wait_recv()
    norm_rows(far_peer)

    def columns(o):
        return nrm[:, pl.ds(pl.multiple_of(o * kb, kb), kb)]

    def project_conv(s):
        for o in owners(s):
            res = jnp.dot(columns(o), wc[rows(o, kb), :], preferred_element_type=F32)
            accc[...] = res if s == 0 else accc[...] + res

    def project_heads(s):
        for o in owners(s):
            lhs = columns(o)
            res = jnp.dot(lhs, wq[o, 0:kb, :], preferred_element_type=F32)
            two = lax.dot_general(
                lhs, wq[o, kb : kb + kvw, :], (((1,), (1,)), ((), ())),
                preferred_element_type=F32,
            )
            if s == 0:
                accq[:, 0:qwidth] = res
                accq[:, qwidth : qwidth + kvw] = two
            else:
                accq[:, 0:qwidth] = accq[:, 0:qwidth] + res
                accq[:, qwidth : qwidth + kvw] = accq[:, qwidth : qwidth + kvw] + two

    project_conv(0)
    ring_event(1, 4)
    ring_event(0, 1, (1,))
    project_conv(1)
    project_conv(2)
    project_conv(3)
    ring_event(0, 2, (0,))
    ring_last(1)
    project_conv(4)
    pad = 16
    glu[pl.ds(pad, length), :] = (
        (accc[:, 0:chans] * jax.nn.sigmoid(accc[:, chans : 2 * chans])).astype(BF).astype(F32)
    )
    g_up = remote(
        glu.at[pl.ds(length, pad)], glu.at[pl.ds(0, pad)], hsem.at[2], hrec.at[2], {"sp": nxt}
    )
    g_down = remote(
        glu.at[pl.ds(pad, pad)], glu.at[pl.ds(length + pad, pad)], hsem.at[3], hrec.at[3],
        {"sp": prv},
    )
    ring_event(0, 2, (1,))
    ntaps = taps.shape[0]
    off = pad - ntaps // 2
    cstep = 64

    def conv_rows(r0):
        acc = jnp.zeros((cstep, chans), F32) + cbias[...]
        for j in range(ntaps):
            acc = acc + glu[pl.ds(r0 + off + j, cstep), :] * taps[pl.ds(j, 1), :]
        filt[pl.ds(r0, cstep), :] = acc

    nconv = length // cstep
    for i in range(1, nconv - 1):
        conv_rows(i * cstep)
    ring_event(0, 3)
    g_up.wait_recv()
    g_down.wait_recv()

    @pl.when(sp == 0)
    def _():
        glu[pl.ds(0, pad), :] = jnp.zeros((pad, chans), F32)

    @pl.when(sp == n - 1)
    def _():
        glu[pl.ds(length + pad, pad), :] = jnp.zeros((pad, chans), F32)

    conv_rows(0)
    conv_rows((nconv - 1) * cstep)
    lane = lax.broadcasted_iota(jnp.int32, (128, 128), 1)
    for b in range(length // 128):
        f = filt[pl.ds(b * 128, 128), :]
        s1 = jnp.sum(f, axis=-1, keepdims=True)
        s2 = jnp.sum(f * f, axis=-1, keepdims=True)
        tile = jnp.where(lane == 0, s1, jnp.where(lane == 1, s2, 0.0))
        stat[pl.ds(t, 1), :, pl.ds(b * 128, 128)] = jnp.transpose(tile)[None, 0:8, :]
    scp = []
    for e, dev in enumerate((y_peer, far_peer, core_peer)):
        scp.append(remote(stat.at[t], stat.at[t], ssem.at[e], srec.at[e], {"tp": dev}))
    ring_event(2, 1, (0,))
    ring_event(0, 4)
    ring_event(2, 1, (1,))
    project_heads(0)
    project_heads(1)
    project_heads(2)
    for cp in scp:
        cp.wait_recv()
    count = chans * 4
    for b in range(length // 128):
        cols = pl.ds(b * 128, 128)
        tot = (stat[0, :, cols] + stat[1, :, cols] + stat[2, :, cols] + stat[3, :, cols]) / count
        tt = jnp.transpose(jnp.concatenate([tot] * 16, axis=0))
        center = tt[:, 0:1]
        spread = tt[:, 1:2] - center * center
        u = (filt[pl.ds(b * 128, 128), :] - center) * lax.rsqrt(spread + 1e-05)
        u = u * ngain[...] + nbias[...]
        feat[pl.ds(b * 128, 128), 0:chans] = (u * jax.nn.sigmoid(u)).astype(BF)

    project_heads(3)
    ring_last(0)
    project_heads(4)
    qb[...] = accq[:, 0:qwidth].astype(BF)
    band[pl.ds(reach, length), :] = accq[:, qwidth : qwidth + kvw].astype(BF)
    kv_up = remote(
        band.at[pl.ds(length, reach)], band.at[pl.ds(0, reach)], hsem.at[0], hrec.at[0],
        {"sp": nxt},
    )
    kv_down = remote(
        band.at[pl.ds(reach, reach)], band.at[pl.ds(length + reach, reach)], hsem.at[1],
        hrec.at[1], {"sp": prv},
    )
    seq_len = length * n

    def attend(b):
        blk = reach
        span = blk + 2 * reach
        kk = band[pl.ds(b * blk, span), 0:hd]
        vv = band[pl.ds(b * blk, span), hd:kvw]
        ri = lax.broadcasted_iota(jnp.int32, (blk, span), 0)
        ci = lax.broadcasted_iota(jnp.int32, (blk, span), 1)
        kp = sp * length + b * blk - reach + ci
        valid = (ci >= ri) & (ci <= ri + 2 * reach) & (kp >= 0) & (kp < seq_len)
        logs = []
        for h in range(heads):
            q = qb[pl.ds(b * blk, blk), h * hd : (h + 1) * hd]
            s = lax.dot_general(
                q, kk, (((1,), (1,)), ((), ())), preferred_element_type=F32
            ) * hd ** (-0.5)
            s = jnp.where(valid, s, -1e30)
            sk = sink[0:1, h : h + 1]
            top = jnp.maximum(jnp.max(s, axis=-1, keepdims=True), sk)
            e = jnp.where(valid, jnp.exp(s - top), 0.0)
            total = jnp.sum(e, axis=-1, keepdims=True) + jnp.exp(sk - top)
            p = (e * (1.0 / total)).astype(BF)
            a = jnp.dot(p, vv, preferred_element_type=F32).astype(BF)
            feat[pl.ds(b * blk, blk), chans + h * hd : chans + (h + 1) * hd] = a
            logs.append(top + jnp.log(total))
        wide = jnp.zeros((blk, 128), F32)
        for h in range(heads):
            wide = jnp.where(lane == h, logs[h], wide)
        logt[:, pl.ds(b * blk, blk)] = jnp.transpose(wide)[0:heads, :]

    nblk = length // reach
    attend(1)
    ring_event(2, 2)
    for b in range(2, nblk - 1):
        attend(b)
    kv_up.wait_recv()
    kv_down.wait_recv()
    attend(0)
    attend(nblk - 1)

    acp, bcp = {}, {}
    order = []

    def emit(o):
        i = len(order)
        order.append(o)
        part[...] = jnp.dot(feat[...], wo[o], preferred_element_type=F32)
        p1s[i, pl.ds(0, tl), :] = part[rows(core_peer, tl), :].astype(BF)
        p1s[i, pl.ds(tl, tl), :] = part[rows(far_peer, tl), :].astype(BF)
        acp[i] = remote(p1s.at[i], p1r.at[i], asem.at[i], arec.at[i], {"tp": core_peer})
        own[i, pl.ds(0, tl), :] = part[rows(t, tl), :]
        own[i, pl.ds(tl, tl), :] = part[rows(y_peer, tl), :]

    def cross(i):
        acp[i].wait_recv()
        p2s[i] = (own[i, pl.ds(tl, tl), :] + p1r[i, pl.ds(tl, tl), :].astype(F32)).astype(BF)
        bcp[i] = remote(p2s.at[i], p2r.at[i], bsem.at[i], brec.at[i], {"tp": y_peer})

    def finish(i):
        bcp[i].wait_recv()
        mixed[:, rows(order[i], ob)] = (
            own[i, pl.ds(0, tl), :] + p1r[i, pl.ds(0, tl), :].astype(F32)
            + p2r[i].astype(F32)
        ).astype(BF)

    def out_step(s):
        for o in owners(s):
            emit(o)
            if len(order) >= 2:
                cross(len(order) - 2)

    out_step(0)
    ring_event(2, 3)
    out_step(1)
    out_step(2)
    ring_event(2, 4)
    out_step(3)
    ring_last(2)
    out_step(half)
    cross(n - 1)
    for i in range(n):
        finish(i)
    for cp in sent:
        cp.wait_send()


def layer(
    n, parts, tokens, in_gain, w_conv_val, w_conv_gate, w_query, w_key, value_weight, conv_taps,
    conv_bias, norm_gain, norm_bias, head_sink_logit, w_out_conv, w_out_attn,
):
    tl, width = tokens.shape
    kb, chans = w_conv_val.shape
    qwidth = w_query.shape[1]
    kvw = 2 * w_key.shape[1]
    heads = head_sink_logit.shape[0]
    ob = w_out_conv.shape[1]
    fits = (
        parts == 4 and n == 8 and tl % 128 == 0 and kb % 128 == 0 and ob % 128 == 0
        and chans % 128 == 0 and kvw == 128 and kb == qwidth and qwidth == heads * kvw // 2
        and conv_taps.shape[0] <= 33
    )
    if not fits:
        return on_device(
            tokens, in_gain, w_conv_val, w_conv_gate, w_query, w_key, value_weight, conv_taps,
            conv_bias, norm_gain, norm_bias, head_sink_logit, w_out_conv, w_out_attn,
        )
    length = 4 * tl
    half = n // 2
    vm = pl.BlockSpec(memory_space=pltpu.VMEM)
    hb = pl.BlockSpec(memory_space=pl.ANY)
    dma = pltpu.SemaphoreType.DMA
    mixed, log_rows = pl.pallas_call(
        functools.partial(fused_kernel, n),
        out_shape=(
            jax.ShapeDtypeStruct((tl, width), BF),
            jax.ShapeDtypeStruct((heads, length), F32),
        ),
        in_specs=[hb, vm, hb, hb, hb, hb, hb, vm, vm, vm, vm, vm, hb, hb],
        out_specs=(vm, vm),
        scratch_shapes=[
            pltpu.VMEM((length, width), BF),
            pltpu.VMEM((length, width), BF),
            pltpu.VMEM((n, kb + kvw, qwidth), BF),
            pltpu.VMEM((n * kb, 2 * chans), BF),
            pltpu.VMEM((n, chans + qwidth, ob), BF),
            pltpu.VMEM((length, qwidth + kvw), F32),
            pltpu.VMEM((length, 2 * chans), F32),
            pltpu.VMEM((length, qwidth), BF),
            pltpu.VMEM((length + 2 * WINDOW_REACH, kvw), BF),
            pltpu.VMEM((length + 32, chans), F32),
            pltpu.VMEM((length, chans), F32),
            pltpu.VMEM((4, 8, length), F32),
            pltpu.VMEM((length, chans + qwidth), BF),
            pltpu.VMEM((length, ob), F32),
            pltpu.VMEM((n, 2 * tl, ob), BF),
            pltpu.VMEM((n, 2 * tl, ob), BF),
            pltpu.VMEM((n, tl, ob), BF),
            pltpu.VMEM((n, tl, ob), BF),
            pltpu.VMEM((n, 2 * tl, ob), F32),
            dma((8,)),
            dma((3, 2)),
            dma((3, 2)),
            dma((3, 2, half, 2)),
            dma((3, 2, half, 2)),
            dma((4,)),
            dma((4,)),
            dma((3,)),
            dma((3,)),
            dma((n,)),
            dma((n,)),
            dma((n,)),
            dma((n,)),
        ],
        compiler_params=pltpu.CompilerParams(
            collective_id=0, has_side_effects=True, vmem_limit_bytes=56 * 1024 * 1024
        ),
    )(
        tokens, in_gain.reshape(1, width), w_conv_val, w_conv_gate, w_query, w_key.T, value_weight.T,
        conv_taps, conv_bias.reshape(1, chans), norm_gain.reshape(1, chans), norm_bias.reshape(1, chans),
        head_sink_logit.reshape(1, heads), w_out_conv, w_out_attn,
    )
    return mixed, log_rows.T


def solution(mesh):
    return jax.shard_map(
        functools.partial(layer, mesh.shape["sp"], mesh.shape["tp"]),
        mesh=mesh,
        in_specs=(
            P(("sp", "tp"), None),
            P(),
            P("sp", "tp"),
            P("sp", "tp"),
            P("sp", "tp"),
            P("sp", "tp"),
            P("sp", "tp"),
            P(None, "tp"),
            P("tp"),
            P("tp"),
            P("tp"),
            P("tp"),
            P("tp", "sp"),
            P("tp", "sp"),
        ),
        out_specs=(P(("sp", "tp"), None), P("sp", "tp")),
        check_vma=False,
    )
```
